32 devices in a mesh: fs: 8 (over z, x), tp: 4 (over y, core).
Axes of the slice: x: 2, y: 2, z: 4, core: 2. Of those that a mesh axis runs over, the one named last changes fastest.
Arguments:
- inputs: bfloat16 [8192, 2048], P('fs'), may hold values from -6 to 6
- cotangents: bfloat16 [8192, 3, 1024], P('fs', None, 'tp'), may hold values from -0.06591797 to 0.06591797
- factors: bfloat16 [3, 2048, 256], P(None, 'fs'), may hold values from -13.810679 to 13.810679
- first_moment: float32 [3, 256, 1024], P(None, None, 'tp'), may hold values from -6 to 6
- second_moment: float32 [3, 256, 1024], P(None, None, 'tp'), may hold values from 0.05 to 1
- master: float32 [3, 2048, 1024], P(None, 'fs', 'tp'), may hold values from -0.125 to 0.125
Outputs:
- update_step: float32 [3, 2048, 1024], P(None, 'fs', 'tp')
- new_master: float32 [3, 2048, 1024], P(None, 'fs', 'tp')
- new_copy: bfloat16 [3, 2048, 1024], P(None, None, 'tp')
- new_first: float32 [3, 256, 1024], P(None, None, 'tp')
- new_second: float32 [3, 256, 1024], P(None, None, 'tp')
The draws below stay inside these ranges and needn't reach their ends.
All inputs are finite; a program needn't handle non-finite values.
Results may differ from the reference program's by a relative error of at most 0.001.
Values may be sent and summed in bfloat16 or wider, within the bound.
A program may use at most 64 MiB of HBM per device.

```python
import math
import jax
import jax.numpy as jnp
from jax import lax

D = 2048
MW = 1024
RANK = 256
MATS = 3
TOKENS = 8192


def draw_factors(key, part):
    keys = jax.random.split(jax.random.fold_in(key, 17), 3)
    position = jnp.arange(D, dtype=jnp.float32) / (D - 1)
    base = jnp.clip(jax.random.normal(keys[0], (MATS, D, RANK), jnp.float32), -5.0, 5.0)
    ramp = jnp.exp(math.log(5.0) * position)
    row_scale = jnp.exp(jax.random.uniform(keys[1], (MATS, D, 1), jnp.float32, 0.0, math.log(10.0)))
    col_scale = jnp.exp(jax.random.uniform(keys[2], (MATS, 1, RANK), jnp.float32, 0.0, math.log(10.0)))
    value = base * ramp[None, :, None] * row_scale * col_scale / (8.0 * math.sqrt(D))
    return value.astype(jnp.bfloat16)


def strengthened(values, stream_key, source, target, parts, factor):
    def block_of(axis_at):
        return (jnp.arange(values.shape[axis_at]) // (values.shape[axis_at] // parts)).reshape((-1,) + (1,) * (values.ndim - 1 - axis_at))

    one_side = jax.random.permutation(stream_key, parts)[block_of(target)]
    far = (block_of(target) + parts // 2) % parts
    return jnp.where((block_of(source) == one_side) | (block_of(source) == far), factor * values, values)


def block_levels(key, dims, pieces, least, high):
    factor_of = 1.0
    for dim, parts in pieces:
        heights = jax.random.uniform(jax.random.fold_in(jax.random.fold_in(key, 6), dim), (parts,), jnp.float32, least / len(pieces), high / len(pieces))
        factor_of = factor_of * jnp.repeat(jnp.exp(heights), dims[dim] // parts).reshape((-1,) + (1,) * (len(dims) - 1 - dim))
    return factor_of


def normal_values(rng, shape, deviation, bound, cuts=(), held_as=jnp.bfloat16):
    values = deviation * jax.random.normal(rng, shape, jnp.float32)
    if cuts:
        values = values * block_levels(rng, shape, cuts, -0.22, 0.18)
    return jnp.clip(values, -bound, bound).astype(held_as)


def noise_with(rng, shape, spread, limit, cuts, heavy, kind=jnp.bfloat16):
    entries = spread * jax.random.normal(rng, shape, jnp.float32)
    if cuts:
        entries = entries * block_levels(rng, shape, cuts, -0.22, 0.18)
    return jnp.clip(strengthened(entries, jax.random.fold_in(rng, 3), *heavy), -limit, limit).astype(kind)


def setup_inputs(seed: int = 0) -> dict:
    streams_of = jax.random.split(jax.random.key(seed), 7)
    inputs = noise_with(streams_of[0], (TOKENS, D), 1.0, 6.0, ((0, 8),), (0, 1, 8, 2.0))
    cotangents = normal_values(streams_of[1], (TOKENS, MATS, MW), (1.0 / TOKENS ** 0.5), 0.06591797, ((0, 8), (2, 4)))
    factors = draw_factors(jax.random.fold_in(streams_of[6], 71), 0)
    first_moment = normal_values(streams_of[3], (MATS, RANK, MW), 1.0, 6.0, ((2, 4),), jnp.float32)
    second_moment = jnp.clip(jnp.exp(math.log(1.0) - 2.9957323 * jax.random.uniform(streams_of[4], (MATS, RANK, MW), jnp.float32) ** block_levels(streams_of[4], (MATS, RANK, MW), ((2, 4),), -0.2, 0.2)), 0.05, 1.0)
    master = normal_values(streams_of[5], (MATS, D, MW), D ** -0.5, 0.125, ((1, 8), (2, 4)), jnp.float32)
    return {"inputs": inputs, "cotangents": cotangents, "factors": factors, "first_moment": first_moment, "second_moment": second_moment, "master": master}


beta_first = 0.8
beta_second = 0.9
adam_eps = 1e-08
norm_eps = 1e-06
learning_rate = 0.005

def reference(inputs, cotangents, factors, first_moment, second_moment, master):
    flat_cot = cotangents.reshape(cotangents.shape[0], MATS * MW)
    gradient = lax.dot_general(inputs, flat_cot, (((0,), (0,)), ((), ())), preferred_element_type=jnp.float32)
    gradient = gradient.reshape(D, MATS, MW).transpose(1, 0, 2)
    factor32 = factors.astype(jnp.float32)
    projected = jnp.einsum('mdr,mdc->mrc', factor32, gradient, precision=lax.Precision.HIGHEST)
    new_first = beta_first * first_moment + (1.0 - beta_first) * projected
    new_second = beta_second * second_moment + (1.0 - beta_second) * projected * projected
    normed = new_first / (jnp.sqrt(new_second) + adam_eps)
    update = jnp.einsum('mdr,mrc->mdc', factor32, normed, precision=lax.Precision.HIGHEST)
    root_mean = jnp.sqrt(lax.optimization_barrier(jnp.mean(update * update, axis=(1, 2))) + norm_eps)
    update_step = update / root_mean[:, None, None]
    new_master = master - learning_rate * update_step
    new_copy = new_master.astype(jnp.bfloat16)
    return (update_step, new_master, new_copy, new_first, new_second)
```

```python
import functools

import jax
import jax.numpy as jnp
from jax import lax
from jax.experimental import pallas as pl
from jax.experimental.pallas import tpu as pltpu
from jax.sharding import PartitionSpec as P

beta_first = 0.8
beta_second = 0.9
adam_eps = 1e-08
norm_eps = 1e-06
learning_rate = 0.005

F32 = jnp.float32
BF16 = jnp.bfloat16


def split2(value):
    high = value.astype(BF16)
    low = (value - high.astype(F32)).astype(BF16)
    return high, low


def kernel(n, tp, width, x_hbm, cot_hbm, fac_hbm, first_hbm, second_hbm, master_hbm,
           step_out, newm_out, copy_out, nf_out, ns_out,
           x, cot, fg, first, second, master, part, got_pair, half_buf, got_line, full,
           step_v, newm_v, copy_v, nf_v, ns_v, upd, sq_mine, sq_all,
           in_sem, out_sem, f_send, f_recv, pair_send, pair_recv, rs_send, rs_recv,
           ag_send, ag_recv, sq_send, sq_recv, c_send, c_recv):
    mats, rows, rank = fac_hbm.shape
    depth = n * rows
    lines = n // 2
    half_rows = rows // 2
    half_rank = rank // 2
    me = lax.axis_index("fs")
    mt = lax.axis_index("tp")
    side = lax.rem(me, 2)
    q = me // 2
    partner = me + 1 - 2 * side
    core = lax.rem(mt, 2)
    mate = mt + 1 - 2 * core

    def remote(src, dst, ssem, rsem, fs=None, t=None):
        return pltpu.make_async_remote_copy(
            src_ref=src, dst_ref=dst, send_sem=ssem, recv_sem=rsem,
            device_id={"fs": me if fs is None else fs, "tp": mt if t is None else t},
            device_id_type=pl.DeviceIdType.MESH)

    my_rows = pl.ds(pl.multiple_of(me * rows, rows), rows)
    load_f = pltpu.make_async_copy(fac_hbm, fg.at[:, my_rows, :], in_sem.at[0])
    load_f.start()
    load_x = pltpu.make_async_copy(x_hbm, x, in_sem.at[1])
    load_x.start()
    load_c = pltpu.make_async_copy(cot_hbm, cot, in_sem.at[2])
    load_c.start()
    load_rest = [pltpu.make_async_copy(a, b, in_sem.at[3 + i]) for i, (a, b) in enumerate(
        ((first_hbm, first), (second_hbm, second), (master_hbm, master)))]
    for copy in load_rest:
        copy.start()

    barrier = pltpu.get_barrier_semaphore()
    for other in range(lines):
        @pl.when(other != q)
        def _():
            pl.semaphore_signal(barrier, inc=1, device_id={"fs": 2 * other + side, "tp": mt},
                                device_id_type=pl.DeviceIdType.MESH)
    pl.semaphore_signal(barrier, inc=1, device_id={"fs": partner, "tp": mt},
                        device_id_type=pl.DeviceIdType.MESH)
    for off in range(1, tp):
        pl.semaphore_signal(barrier, inc=1, device_id={"fs": me, "tp": lax.rem(mt + off, tp)},
                            device_id_type=pl.DeviceIdType.MESH)
    pl.semaphore_wait(barrier, lines - 1 + 1 + tp - 1)
    load_f.wait()

    def f_piece(m, fs, which):
        start = pl.multiple_of(fs * rows + which * half_rows, half_rows)
        return fg.at[m, pl.ds(start, half_rows), :]

    def f_copy(m, fs, kind, which=None):
        ref = f_piece(m, fs, core if which is None else which)
        if kind == 0:
            target = dict(fs=me - 2)
        elif kind == 1:
            target = dict(fs=me + 2)
        elif kind == 2:
            target = dict(fs=partner)
        else:
            target = dict(t=mate)
        slot = (core if which is None else which)
        return remote(ref, ref, f_send.at[m, fs, kind], f_recv.at[m, fs, slot], **target)

    def line_forward(copy_of, m, extra):
        for dist in range(1, lines):
            @pl.when(q >= dist)
            def _():
                src = me - 2 * dist
                copy_of(m, src, 1).wait_recv()

                @pl.when(q < lines - 1)
                def _():
                    copy_of(m, src, 1).start()
                copy_of(m, src, 2).start()
                if extra:
                    copy_of(m, src, 3).start()

            @pl.when(q + dist < lines)
            def _():
                src = me + 2 * dist
                copy_of(m, src, 0).wait_recv()

                @pl.when(q > 0)
                def _():
                    copy_of(m, src, 0).start()
                copy_of(m, src, 2).start()
                if extra:
                    copy_of(m, src, 3).start()

    def own_sends(copy_of, m):
        @pl.when(q < lines - 1)
        def _():
            copy_of(m, me, 1).start()

        @pl.when(q > 0)
        def _():
            copy_of(m, me, 0).start()
        copy_of(m, me, 2).start()

    def pair_arrivals(copy_of, m, extra):
        order = [0]
        for dist in range(1, lines):
            order += [-dist, dist]
        for dist in order:
            @pl.when((q + dist >= 0) & (q + dist < lines))
            def _():
                src = partner + 2 * dist
                copy_of(m, src, 2).wait_recv()
                if extra:
                    copy_of(m, src, 3).start()

    def drain(copy_of, m, extra):
        for dist in range(-(lines - 1), lines):
            if dist == 0:
                @pl.when(q < lines - 1)
                def _():
                    copy_of(m, me, 1).wait_send()

                @pl.when(q > 0)
                def _():
                    copy_of(m, me, 0).wait_send()
                copy_of(m, me, 2).wait_send()
                if extra:
                    copy_of(m, partner, 3).wait_send()
                continue

            @pl.when((q + dist >= 0) & (q + dist < lines))
            def _():
                src = me + 2 * dist
                if dist < 0:
                    @pl.when(q < lines - 1)
                    def _():
                        copy_of(m, src, 1).wait_send()
                else:
                    @pl.when(q > 0)
                    def _():
                        copy_of(m, src, 0).wait_send()
                copy_of(m, src, 2).wait_send()
                if extra:
                    copy_of(m, src, 3).wait_send()
                    copy_of(m, partner + 2 * dist, 3).wait_send()

    def mate_arrivals(m):
        for dist in range(1, n):
            src = lax.rem(me + dist, n)
            f_copy(m, src, 3, 1 - core).wait_recv()

    def f_gather(m):
        line_forward(f_copy, m, True)
        pair_arrivals(f_copy, m, True)
        mate_arrivals(m)

    def partial_of(m):
        lowered = jnp.dot(x[...], fg[m], preferred_element_type=F32)
        high, low = split2(lowered)
        c = cot[:, m, :]
        dims = (((0,), (0,)), ((), ()))
        value = lax.dot_general(high, c, dims, preferred_element_type=F32)
        value = value + lax.dot_general(low, c, dims, preferred_element_type=F32)
        part[m, 0] = value[:half_rank]
        part[m, 1] = value[half_rank:]

    def pair_copy(m):
        return remote(part.at[m, 1 - side], got_pair.at[m], pair_send.at[m], pair_recv.at[m], fs=partner)

    def rs_copy(m, other, slot):
        return remote(half_buf.at[m, other], got_line.at[m, slot], rs_send.at[m, other],
                      rs_recv.at[m, slot], fs=2 * other + side)

    def ag_copy(m, other, slot):
        ref = full.at[m, side, slot]
        return remote(ref, ref, ag_send.at[m, other], ag_recv.at[m, side, slot], fs=2 * other + side)

    def ag_pair(m, slot, arriving=False):
        s = 1 - side if arriving else side
        ref = full.at[m, s, slot]
        return remote(ref, ref, ag_send.at[m, lines + slot], ag_recv.at[m, s, slot], fs=partner)

    piece = half_rank // lines

    def rs_line(m):
        pair_copy(m).wait_recv()
        total = part[m, side] + got_pair[m]
        for j in range(lines):
            half_buf[m, j] = total[j * piece:(j + 1) * piece]
        for off in range(1, lines):
            other = lax.rem(q + off, lines)
            rs_copy(m, other, q).start()

    def rs_end(m):
        total = half_buf[m, q]
        for off in range(1, lines):
            src = lax.rem(q + off, lines)
            rs_copy(m, q, src).wait_recv()
            total = total + got_line[m, src]
        full[m, side, q] = total
        for off in range(1, lines):
            other = lax.rem(q + off, lines)
            ag_copy(m, other, q).start()
        ag_pair(m, q).start()

    def ag_forward(m):
        for off in range(1, lines):
            src = lax.rem(q + off, lines)
            ag_copy(m, q, src).wait_recv()
            ag_pair(m, src).start()

    def finish(m):
        for off in range(lines):
            ag_pair(m, lax.rem(q + off, lines), True).wait_recv()
        if m == 0:
            for copy in load_rest:
                copy.wait()
        projected = jnp.concatenate(
            [full[m, s, j] for s in range(2) for j in range(lines)], axis=0)
        nf = beta_first * first[m] + (1.0 - beta_first) * projected
        ns = beta_second * second[m] + (1.0 - beta_second) * projected * projected
        nf_v[m] = nf
        ns_v[m] = ns
        normed = nf / (jnp.sqrt(ns) + adam_eps)
        high, low = split2(normed)
        upd[m] = (jnp.dot(fg[m], high, preferred_element_type=F32)
                  + jnp.dot(fg[m], low, preferred_element_type=F32))
        value = upd[m]
        squares = jnp.sum(value * value)
        sq_mine[m] = jnp.full(sq_mine.shape[1:], squares, F32)
        sq_all[m, mt] = jnp.full(sq_mine.shape[1:], squares, F32)
        for off in range(1, tp):
            sq_copy(m, lax.rem(mt + off, tp), mt).start()
        pltpu.make_async_copy(nf_v.at[m], nf_out.at[m], out_sem.at[0, m]).start()
        pltpu.make_async_copy(ns_v.at[m], ns_out.at[m], out_sem.at[1, m]).start()

    def sq_copy(m, other, slot):
        return remote(sq_mine.at[m], sq_all.at[m, slot], sq_send.at[m, other], sq_recv.at[m, slot], t=other)

    def c_copy(m, fs, kind):
        ref = copy_v.at[m, pl.ds(pl.multiple_of(fs * rows, rows), rows), :]
        target = (me - 2, me + 2, partner)[kind]
        return remote(ref, ref, c_send.at[m, fs, kind], c_recv.at[m, fs], fs=target)

    def scale(m):
        for off in range(1, tp):
            src = lax.rem(mt + off, tp)
            sq_copy(m, mt, src).wait_recv()
        total = sq_all[m, 0]
        for t in range(1, tp):
            total = total + sq_all[m, t]
        root = jnp.sqrt(total[0:1, 0:1] / (depth * width) + norm_eps)
        step = upd[m, my_rows, :] / root
        new = master[m] - learning_rate * step
        copy_v[m, my_rows, :] = new.astype(BF16)
        own_sends(c_copy, m)
        step_v[m] = step
        newm_v[m] = new
        pltpu.make_async_copy(step_v.at[m], step_out.at[m], out_sem.at[2, m]).start()
        pltpu.make_async_copy(newm_v.at[m], newm_out.at[m], out_sem.at[3, m]).start()

    def copy_end(m):
        pair_arrivals(c_copy, m, False)
        pltpu.make_async_copy(copy_v.at[m], copy_out.at[m], out_sem.at[4, m]).start()

    for m in range(mats):
        own_sends(f_copy, m)
    for t in range(mats + 8):
        def at(stage, func):
            m = t - stage
            if 0 <= m < mats:
                func(m)
        at(0, f_gather)
        if t == 0:
            load_x.wait()
            load_c.wait()
        at(0, partial_of)
        at(0, lambda m: pair_copy(m).start())
        at(2, rs_end)
        at(1, rs_line)
        at(3, ag_forward)
        at(3, finish)
        at(4, scale)
        at(5, lambda m: line_forward(c_copy, m, False))
        at(6, copy_end)

    for m in range(mats):
        drain(f_copy, m, True)
        pair_copy(m).wait_send()
        for off in range(1, lines):
            other = lax.rem(q + off, lines)
            rs_copy(m, other, q).wait_send()
            ag_copy(m, other, q).wait_send()
        for slot in range(lines):
            ag_pair(m, slot).wait_send()
        for off in range(1, tp):
            sq_copy(m, lax.rem(mt + off, tp), mt).wait_send()
        drain(c_copy, m, False)
        for i, (a, b) in enumerate(((nf_v, nf_out), (ns_v, ns_out), (step_v, step_out), (newm_v, newm_out), (copy_v, copy_out))):
            pltpu.make_async_copy(a.at[m], b.at[m], out_sem.at[i, m]).wait()


def local(n, tp, inputs, cotangents, factors, first_moment, second_moment, master):
    tokens, depth = inputs.shape
    mats, rows, rank = factors.shape
    cols = cotangents.shape[2]
    lines = n // 2
    piece = rank // 2 // lines
    V = pltpu.VMEM
    dma = pltpu.SemaphoreType.DMA
    anyspec = pl.BlockSpec(memory_space=pl.ANY)
    small = jax.ShapeDtypeStruct((mats, rank, cols), F32)
    shard = jax.ShapeDtypeStruct((mats, rows, cols), F32)
    return pl.pallas_call(
        functools.partial(kernel, n, tp, cols * tp),
        out_shape=(shard, shard, jax.ShapeDtypeStruct((mats, depth, cols), BF16), small, small),
        in_specs=[anyspec] * 6,
        out_specs=(anyspec,) * 5,
        scratch_shapes=[
            V(inputs.shape, BF16), V(cotangents.shape, BF16), V((mats, depth, rank), BF16),
            V(small.shape, F32), V(small.shape, F32), V(shard.shape, F32),
            V((mats, 2, rank // 2, cols), F32), V((mats, rank // 2, cols), F32),
            V((mats, lines, piece, cols), F32), V((mats, lines, piece, cols), F32),
            V((mats, 2, lines, piece, cols), F32),
            V(shard.shape, F32), V(shard.shape, F32), V((mats, depth, cols), BF16),
            V(small.shape, F32), V(small.shape, F32), V((mats, depth, cols), F32),
            V((mats, 8, 128), F32), V((mats, tp, 8, 128), F32),
            dma((6,)), dma((5, mats)), dma((mats, n, 4)), dma((mats, n, 2)),
            dma((mats,)), dma((mats,)), dma((mats, lines)), dma((mats, lines)),
            dma((mats, 2 * lines)), dma((mats, 2, lines)), dma((mats, tp)), dma((mats, tp)),
            dma((mats, n, 3)), dma((mats, n)),
        ],
        compiler_params=pltpu.CompilerParams(
            collective_id=0, has_side_effects=True, vmem_limit_bytes=60 * 2 ** 20),
    )(inputs, cotangents, factors, first_moment, second_moment, master)


def solution(mesh):
    placed = (
        P("fs", None),
        P("fs", None, "tp"),
        P(None, "fs", None),
        P(None, None, "tp"),
        P(None, None, "tp"),
        P(None, "fs", "tp"),
    )
    return jax.shard_map(
        functools.partial(local, mesh.shape["fs"], mesh.shape["tp"]),
        mesh=mesh,
        in_specs=placed,
        out_specs=(
            P(None, "fs", "tp"),
            P(None, "fs", "tp"),
            P(None, None, "tp"),
            P(None, None, "tp"),
            P(None, None, "tp"),
        ),
        check_vma=False,
    )
```

```python
import functools

import jax
import jax.numpy as jnp
from jax import lax
from jax.experimental import pallas as pl
from jax.experimental.pallas import tpu as pltpu
from jax.sharding import PartitionSpec as P

beta_first = 0.8
beta_second = 0.9
adam_eps = 1e-08
norm_eps = 1e-06
learning_rate = 0.005

F32 = jnp.float32
BF16 = jnp.bfloat16


def split2(value):
    high = value.astype(BF16)
    low = (value - high.astype(F32)).astype(BF16)
    return high, low


def kernel(n, tp, width, x_hbm, cot_hbm, fac_hbm, first_hbm, second_hbm, master_hbm,
           step_v, newm_v, copy_v, nf_v, ns_v,
           x, cot, fg, first, second, master, part, got_pair, half_buf, got_line, full,
           upd, sq_mine, sq_all,
           in_sem, f_send, f_recv, pair_send, pair_recv, rs_send, rs_recv,
           ag_send, ag_recv, sq_send, sq_recv, c_send, c_recv):
    mats, rows, rank = fac_hbm.shape
    depth = n * rows
    lines = n // 2
    half_rows = rows // 2
    half_rank = rank // 2
    me = lax.axis_index("fs")
    mt = lax.axis_index("tp")
    side = lax.rem(me, 2)
    q = me // 2
    partner = me + 1 - 2 * side
    core = lax.rem(mt, 2)
    mate = mt + 1 - 2 * core

    def remote(src, dst, ssem, rsem, fs=None, t=None):
        return pltpu.make_async_remote_copy(
            src_ref=src, dst_ref=dst, send_sem=ssem, recv_sem=rsem,
            device_id={"fs": me if fs is None else fs, "tp": mt if t is None else t},
            device_id_type=pl.DeviceIdType.MESH)

    my_rows = pl.ds(pl.multiple_of(me * rows, rows), rows)
    load_f = pltpu.make_async_copy(fac_hbm, fg.at[:, my_rows, :], in_sem.at[0])
    load_f.start()
    load_x = pltpu.make_async_copy(x_hbm, x, in_sem.at[1])
    load_x.start()
    load_c = pltpu.make_async_copy(cot_hbm, cot, in_sem.at[2])
    load_c.start()
    load_rest = [pltpu.make_async_copy(a, b, in_sem.at[3 + i]) for i, (a, b) in enumerate(
        ((first_hbm, first), (second_hbm, second), (master_hbm, master)))]
    for copy in load_rest:
        copy.start()

    barrier = pltpu.get_barrier_semaphore()
    for other in range(lines):
        @pl.when(other != q)
        def _():
            pl.semaphore_signal(barrier, inc=1, device_id={"fs": 2 * other + side, "tp": mt},
                                device_id_type=pl.DeviceIdType.MESH)
    pl.semaphore_signal(barrier, inc=1, device_id={"fs": partner, "tp": mt},
                        device_id_type=pl.DeviceIdType.MESH)
    for off in range(1, tp):
        pl.semaphore_signal(barrier, inc=1, device_id={"fs": me, "tp": lax.rem(mt + off, tp)},
                            device_id_type=pl.DeviceIdType.MESH)
    pl.semaphore_wait(barrier, lines - 1 + 1 + tp - 1)
    load_f.wait()

    def f_piece(m, fs, which):
        start = pl.multiple_of(fs * rows + which * half_rows, half_rows)
        return fg.at[m, pl.ds(start, half_rows), :]

    def f_copy(m, fs, kind, which=None):
        ref = f_piece(m, fs, core if which is None else which)
        if kind == 0:
            target = dict(fs=me - 2)
        elif kind == 1:
            target = dict(fs=me + 2)
        elif kind == 2:
            target = dict(fs=partner)
        else:
            target = dict(t=mate)
        slot = (core if which is None else which)
        return remote(ref, ref, f_send.at[m, fs, kind], f_recv.at[m, fs, slot], **target)

    def line_forward(copy_of, m, extra):
        for dist in range(1, lines):
            @pl.when(q >= dist)
            def _():
                src = me - 2 * dist
                copy_of(m, src, 1).wait_recv()

                @pl.when(q < lines - 1)
                def _():
                    copy_of(m, src, 1).start()
                copy_of(m, src, 2).start()
                if extra:
                    copy_of(m, src, 3).start()

            @pl.when(q + dist < lines)
            def _():
                src = me + 2 * dist
                copy_of(m, src, 0).wait_recv()

                @pl.when(q > 0)
                def _():
                    copy_of(m, src, 0).start()
                copy_of(m, src, 2).start()
                if extra:
                    copy_of(m, src, 3).start()

    def own_sends(copy_of, m):
        @pl.when(q < lines - 1)
        def _():
            copy_of(m, me, 1).start()

        @pl.when(q > 0)
        def _():
            copy_of(m, me, 0).start()
        copy_of(m, me, 2).start()

    def pair_arrivals(copy_of, m, extra):
        order = [0]
        for dist in range(1, lines):
            order += [-dist, dist]
        for dist in order:
            @pl.when((q + dist >= 0) & (q + dist < lines))
            def _():
                src = partner + 2 * dist
                copy_of(m, src, 2).wait_recv()
                if extra:
                    copy_of(m, src, 3).start()

    def drain(copy_of, m, extra):
        for dist in range(-(lines - 1), lines):
            if dist == 0:
                @pl.when(q < lines - 1)
                def _():
                    copy_of(m, me, 1).wait_send()

                @pl.when(q > 0)
                def _():
                    copy_of(m, me, 0).wait_send()
                copy_of(m, me, 2).wait_send()
                if extra:
                    copy_of(m, partner, 3).wait_send()
                continue

            @pl.when((q + dist >= 0) & (q + dist < lines))
            def _():
                src = me + 2 * dist
                if dist < 0:
                    @pl.when(q < lines - 1)
                    def _():
                        copy_of(m, src, 1).wait_send()
                else:
                    @pl.when(q > 0)
                    def _():
                        copy_of(m, src, 0).wait_send()
                copy_of(m, src, 2).wait_send()
                if extra:
                    copy_of(m, src, 3).wait_send()
                    copy_of(m, partner + 2 * dist, 3).wait_send()

    def mate_arrivals(m):
        for dist in range(1, n):
            src = lax.rem(me + dist, n)
            f_copy(m, src, 3, 1 - core).wait_recv()

    def f_gather(m):
        line_forward(f_copy, m, True)
        pair_arrivals(f_copy, m, True)
        mate_arrivals(m)

    def partial_of(m):
        lowered = jnp.dot(x[...], fg[m], preferred_element_type=F32)
        high, low = split2(lowered)
        c = cot[m]
        dims = (((0,), (0,)), ((), ()))
        value = lax.dot_general(high, c, dims, preferred_element_type=F32)
        value = value + lax.dot_general(low, c, dims, preferred_element_type=F32)
        part[m, 0] = value[:half_rank]
        part[m, 1] = value[half_rank:]

    def pair_copy(m):
        return remote(part.at[m, 1 - side], got_pair.at[m], pair_send.at[m], pair_recv.at[m], fs=partner)

    def rs_copy(m, other, slot):
        return remote(half_buf.at[m, other], got_line.at[m, slot], rs_send.at[m, other],
                      rs_recv.at[m, slot], fs=2 * other + side)

    def ag_copy(m, other, slot):
        ref = full.at[m, side, slot]
        return remote(ref, ref, ag_send.at[m, other], ag_recv.at[m, side, slot], fs=2 * other + side)

    def ag_pair(m, slot, arriving=False):
        s = 1 - side if arriving else side
        ref = full.at[m, s, slot]
        return remote(ref, ref, ag_send.at[m, lines + slot], ag_recv.at[m, s, slot], fs=partner)

    piece = half_rank // lines

    def rs_line(m):
        pair_copy(m).wait_recv()
        total = part[m, side] + got_pair[m]
        for j in range(lines):
            half_buf[m, j] = total[j * piece:(j + 1) * piece]
        for off in range(1, lines):
            other = lax.rem(q + off, lines)
            rs_copy(m, other, q).start()

    def rs_end(m):
        total = half_buf[m, q]
        for off in range(1, lines):
            src = lax.rem(q + off, lines)
            rs_copy(m, q, src).wait_recv()
            total = total + got_line[m, src]
        full[m, side, q] = total
        for off in range(1, lines):
            other = lax.rem(q + off, lines)
            ag_copy(m, other, q).start()
        ag_pair(m, q).start()

    def ag_forward(m):
        for off in range(1, lines):
            src = lax.rem(q + off, lines)
            ag_copy(m, q, src).wait_recv()
            ag_pair(m, src).start()

    def finish(m):
        for off in range(lines):
            ag_pair(m, lax.rem(q + off, lines), True).wait_recv()
        if m == 0:
            for copy in load_rest:
                copy.wait()
        projected = jnp.concatenate(
            [full[m, s, j] for s in range(2) for j in range(lines)], axis=0)
        nf = beta_first * first[m] + (1.0 - beta_first) * projected
        ns = beta_second * second[m] + (1.0 - beta_second) * projected * projected
        nf_v[m] = nf
        ns_v[m] = ns
        normed = nf / (jnp.sqrt(ns) + adam_eps)
        high, low = split2(normed)
        upd[m] = (jnp.dot(fg[m], high, preferred_element_type=F32)
                  + jnp.dot(fg[m], low, preferred_element_type=F32))
        value = upd[m]
        squares = jnp.sum(value * value)
        sq_mine[m] = jnp.full(sq_mine.shape[1:], squares, F32)
        sq_all[m, mt] = jnp.full(sq_mine.shape[1:], squares, F32)
        for off in range(1, tp):
            sq_copy(m, lax.rem(mt + off, tp), mt).start()

    def sq_copy(m, other, slot):
        return remote(sq_mine.at[m], sq_all.at[m, slot], sq_send.at[m, other], sq_recv.at[m, slot], t=other)

    def c_copy(m, fs, kind):
        ref = copy_v.at[m, pl.ds(pl.multiple_of(fs * rows, rows), rows), :]
        target = (me - 2, me + 2, partner)[kind]
        return remote(ref, ref, c_send.at[m, fs, kind], c_recv.at[m, fs], fs=target)

    def scale(m):
        for off in range(1, tp):
            src = lax.rem(mt + off, tp)
            sq_copy(m, mt, src).wait_recv()
        total = sq_all[m, 0]
        for t in range(1, tp):
            total = total + sq_all[m, t]
        root = jnp.sqrt(total[0:1, 0:1] / (depth * width) + norm_eps)
        step = upd[m, my_rows, :] / root
        new = master[m] - learning_rate * step
        copy_v[m, my_rows, :] = new.astype(BF16)
        own_sends(c_copy, m)
        step_v[m] = step
        newm_v[m] = new

    def copy_end(m):
        pair_arrivals(c_copy, m, False)

    for m in range(mats):
        own_sends(f_copy, m)
    for t in range(mats + 8):
        def at(stage, func):
            m = t - stage
            if 0 <= m < mats:
                func(m)
        at(0, f_gather)
        if t == 0:
            load_x.wait()
            load_c.wait()
        at(0, partial_of)
        at(0, lambda m: pair_copy(m).start())
        at(2, rs_end)
        at(1, rs_line)
        at(4, scale)
        at(3, ag_forward)
        at(3, finish)
        at(5, lambda m: line_forward(c_copy, m, False))
        at(6, copy_end)

    for m in range(mats):
        drain(f_copy, m, True)
        pair_copy(m).wait_send()
        for off in range(1, lines):
            other = lax.rem(q + off, lines)
            rs_copy(m, other, q).wait_send()
            ag_copy(m, other, q).wait_send()
        for slot in range(lines):
            ag_pair(m, slot).wait_send()
        for off in range(1, tp):
            sq_copy(m, lax.rem(mt + off, tp), mt).wait_send()
        drain(c_copy, m, False)


def write_out(*refs):
    sem = refs[10]
    copies = [pltpu.make_async_copy(refs[i], refs[5 + i], sem.at[i]) for i in range(5)]
    for copy in copies:
        copy.start()
    for copy in copies:
        copy.wait()


def local(n, tp, inputs, cotangents, factors, first_moment, second_moment, master):
    tokens, depth = inputs.shape
    mats, rows, rank = factors.shape
    cols = cotangents.shape[2]
    lines = n // 2
    piece = rank // 2 // lines
    V = pltpu.VMEM
    dma = pltpu.SemaphoreType.DMA
    anyspec = pl.BlockSpec(memory_space=pltpu.HBM)
    small = jax.ShapeDtypeStruct((mats, rank, cols), F32)
    shard = jax.ShapeDtypeStruct((mats, rows, cols), F32)
    held = pl.pallas_call(
        functools.partial(kernel, n, tp, cols * tp),
        out_shape=(V(shard.shape, F32), V(shard.shape, F32), V((mats, depth, cols), BF16),
                   V(small.shape, F32), V(small.shape, F32)),
        in_specs=[anyspec] * 6,
        out_specs=(pl.BlockSpec(memory_space=V),) * 5,
        scratch_shapes=[
            V(inputs.shape, BF16), V((mats, tokens, cols), BF16), V((mats, depth, rank), BF16),
            V(small.shape, F32), V(small.shape, F32), V(shard.shape, F32),
            V((mats, 2, rank // 2, cols), F32), V((mats, rank // 2, cols), F32),
            V((mats, lines, piece, cols), F32), V((mats, lines, piece, cols), F32),
            V((mats, 2, lines, piece, cols), F32),
            V((mats, depth, cols), F32),
            V((mats, 8, 128), F32), V((mats, tp, 8, 128), F32),
            dma((6,)), dma((mats, n, 4)), dma((mats, n, 2)),
            dma((mats,)), dma((mats,)), dma((mats, lines)), dma((mats, lines)),
            dma((mats, 2 * lines)), dma((mats, 2, lines)), dma((mats, tp)), dma((mats, tp)),
            dma((mats, n, 3)), dma((mats, n)),
        ],
        compiler_params=pltpu.CompilerParams(
            collective_id=0, has_side_effects=True, vmem_limit_bytes=36 * 2 ** 20),
    )(inputs, jnp.transpose(cotangents, (1, 0, 2)), factors, first_moment, second_moment, master)
    return pl.pallas_call(
        write_out,
        out_shape=(shard, shard, jax.ShapeDtypeStruct((mats, depth, cols), BF16), small, small),
        in_specs=[pl.BlockSpec(memory_space=V)] * 5,
        out_specs=(anyspec,) * 5,
        scratch_shapes=[dma((5,))],
    )(*held)


def solution(mesh):
    placed = (
        P("fs", None),
        P("fs", None, "tp"),
        P(None, "fs", None),
        P(None, None, "tp"),
        P(None, None, "tp"),
        P(None, "fs", "tp"),
    )
    return jax.shard_map(
        functools.partial(local, mesh.shape["fs"], mesh.shape["tp"]),
        mesh=mesh,
        in_specs=placed,
        out_specs=(
            P(None, "fs", "tp"),
            P(None, "fs", "tp"),
            P(None, None, "tp"),
            P(None, None, "tp"),
            P(None, None, "tp"),
        ),
        check_vma=False,
    )
```
